32 devices in a mesh: grp: 2 (over x), tp: 16 (over z, y, core).
Axes of the slice: x: 2, y: 2, z: 4, core: 2. Of those that a mesh axis runs over, the one named last changes fastest.
Arguments:
- tokens: bfloat16 [2048, 2048], P('grp', 'tp'), parts along dimension 0, may hold values from -8 to 8
- carried: float32 [2, 2, 32, 64, 2048], P(None, None, 'tp', None, 'grp'), parts along dimension 4, may hold values from -3 to 3
- proj_in: bfloat16 [2, 2048, 512], P(None, None, 'tp'), may hold values from -0.125 to 0.125
- proj_gate: bfloat16 [2, 2048, 512], P(None, None, 'tp'), may hold values from -0.125 to 0.125
- proj_out: bfloat16 [2, 512, 2048], P(None, None, 'tp'), may hold values from -0.5 to 0.5
- norm_params: bfloat16 [2, 2, 2048], P(None, None, 'tp'), may hold values from -0.5 to 2.4
- lambda_re: float32 [2, 32, 64], P(None, 'tp'), may hold values from -1 to -0.05
- lambda_im: float32 [2, 32, 64], P(None, 'tp'), may hold values from -3 to 3
- log_step: float32 [2, 32], P(None, 'tp'), may hold values from -3 to 0
- in_coupling: float32 [2, 2, 32, 64, 16], P(None, None, 'tp'), may hold values from -1 to 1
- out_coupling: float32 [2, 2, 32, 16, 64], P(None, None, 'tp'), may hold values from -1.5 to 1.5
- skip_gain: float32 [2, 512], P(None, 'tp'), may hold values from -4 to 4
Outputs:
- stream_out: bfloat16 [2048, 2048], P('grp', 'tp'), parts along dimension 0
- new_carried: float32 [2, 2, 32, 64, 2048], P(None, None, 'tp', None, 'grp'), parts along dimension 4
The draws below stay inside these ranges and needn't reach their ends.
There are 2 independent parts, one for each index of `grp`. The reference program is written for one: setup_inputs(seed, part) draws one part's arguments, and reference() takes and returns one part's arrays. A program takes and returns all parts, laid end to end along the dimension named above; an argument that names none is the same for every part. Nothing has to cross between parts.
All inputs are finite; a program needn't handle non-finite values.
Results may differ from the reference program's by a relative error of at most 0.015.
Values may be sent and summed in bfloat16 or wider, within the bound.
No kernel may reach another device: no remote copies, remote signals or barrier semaphores. Data moves between devices by JAX's collectives and lax.ppermute only.
A program may use at most 64 MiB of HBM per device.

```python
import jax
import jax.numpy as jnp
from jax import lax

D = 2048
GROUPS = 32
GROUP_CH = 16
STATE = 64
SSM = 512
LAYERS = 2
BATCH = 1024


def draw_tokens(key, part):
    keys = jax.random.split(jax.random.fold_in(key, 11), 3)
    base = jax.random.normal(keys[0], (BATCH, D), jnp.float32)
    ramp = jnp.exp(jnp.linspace(jnp.log(0.4), jnp.log(1.6), D)) * jax.random.uniform(keys[1], (D,), jnp.float32, 0.7, 1.3)
    scales = jnp.exp(jax.random.uniform(keys[2], (BATCH, 1), jnp.float32, jnp.log(0.5), jnp.log(2.0)))
    values = base * ramp[None, :] * scales
    return jnp.clip(values, -8.0, 8.0).astype(jnp.bfloat16)


def draw_norm_params(key, part):
    keys = jax.random.split(jax.random.fold_in(key, 23), 2)
    ramp = jnp.exp(jnp.linspace(jnp.log(0.6), jnp.log(1.8), D))
    gains = ramp[None, :] * jax.random.uniform(keys[0], (LAYERS, D), jnp.float32, 0.8, 1.2)
    biases = jax.random.uniform(keys[1], (LAYERS, D), jnp.float32, -0.4, 0.4)
    return jnp.stack([gains, biases], axis=1).astype(jnp.bfloat16)


def steps_of(own_key, extent, pieces, low, top_value):
    factor_of = 1.0
    for dim, shards_of in pieces:
        heights = jax.random.uniform(jax.random.fold_in(jax.random.fold_in(own_key, 6), dim), (shards_of,), jnp.float32, low / len(pieces), top_value / len(pieces))
        factor_of = factor_of * jnp.repeat(jnp.exp(heights), extent[dim] // shards_of).reshape((-1,) + (1,) * (len(extent) - 1 - dim))
    return factor_of


def scatter_about(own_key, shape, spread, reach, cuts=(), held_as=jnp.bfloat16):
    loudness = steps_of(own_key, shape, cuts, -0.22, 0.18) if cuts else 1.0
    array = jax.random.normal(own_key, shape, jnp.float32) * spread * loudness
    return jnp.minimum(jnp.maximum(array, -reach), reach).astype(held_as)


def setup_inputs(seed: int = 0, part: int = 0) -> dict:
    splits = jax.random.split(jax.random.key(seed), 13)
    own_keys = jax.random.split(jax.random.fold_in(splits[12], part), 13)
    tokens = draw_tokens(jax.random.fold_in(jax.random.fold_in(splits[12], part), 71), part)
    carried = scatter_about(own_keys[1], (LAYERS, 2, GROUPS, STATE, BATCH), 0.3, 3.0, ((2, 16),), jnp.float32)
    proj_in = scatter_about(splits[2], (LAYERS, D, SSM), D ** -0.5, 0.125, ((2, 16),))
    proj_gate = scatter_about(splits[3], (LAYERS, D, SSM), D ** -0.5, 0.125, ((2, 16),))
    proj_out = scatter_about(splits[4], (LAYERS, SSM, D), (SSM // 4) ** -0.5, 0.5, ((2, 16),))
    norm_params = draw_norm_params(jax.random.fold_in(splits[12], 71), part)
    lambda_re = jnp.clip(-1.0 + 0.95 * jax.random.uniform(splits[6], (LAYERS, GROUPS, STATE), jnp.float32) ** steps_of(splits[6], (LAYERS, GROUPS, STATE), ((1, 16),), -0.2, 0.2), -1.0, -0.05)
    lambda_im = jnp.clip(jax.random.uniform(splits[7], (LAYERS, GROUPS, STATE), jnp.float32, -3.0, 3.0) * steps_of(splits[7], (LAYERS, GROUPS, STATE), ((1, 16),), -0.4, 0.0), -3.0, 3.0)
    log_step = jnp.clip(-3.0 + 3.0 * jax.random.uniform(splits[8], (LAYERS, GROUPS), jnp.float32) ** steps_of(splits[8], (LAYERS, GROUPS), ((1, 16),), -0.2, 0.2), -3.0, 0.0)
    in_coupling = scatter_about(splits[9], (LAYERS, 2, GROUPS, STATE, GROUP_CH), (2 * GROUP_CH) ** -0.5, 1.0, ((2, 16),), jnp.float32)
    out_coupling = scatter_about(splits[10], (LAYERS, 2, GROUPS, GROUP_CH, STATE), (STATE // 4) ** -0.5, 1.5, ((2, 16),), jnp.float32)
    skip_gain = scatter_about(splits[11], (LAYERS, SSM), 1.0, 4.0, ((1, 16),), jnp.float32)
    return dict(tokens=tokens, carried=carried, proj_in=proj_in, proj_gate=proj_gate, proj_out=proj_out, norm_params=norm_params, lambda_re=lambda_re, lambda_im=lambda_im, log_step=log_step, in_coupling=in_coupling, out_coupling=out_coupling, skip_gain=skip_gain)


residual_scale = 1.4142135623730951
norm_eps = 1e-05
highest_precision = lax.Precision.HIGHEST

def discretize(lam_re, lam_im, log_dt, coupling):
    step_len = jnp.exp(log_dt)[:, None]
    modulus = jnp.exp(lam_re * step_len)
    decay_re = modulus * jnp.cos(lam_im * step_len)
    decay_im = modulus * jnp.sin(lam_im * step_len)
    denominator = lam_re * lam_re + lam_im * lam_im
    shifted = decay_re - 1.0
    coef_re = (shifted * lam_re + decay_im * lam_im) / denominator
    coef_im = (decay_im * lam_re - shifted * lam_im) / denominator
    in_re = coef_re[..., None] * coupling[0] - coef_im[..., None] * coupling[1]
    in_im = coef_re[..., None] * coupling[1] + coef_im[..., None] * coupling[0]
    return (decay_re, decay_im, in_re, in_im)

def recur(drive, gate_pre, states, lam_re, lam_im, log_dt, in_c, output_coupling, skip_connection):
    channel_groups = lam_re.shape[0]
    batch_rows = drive.shape[0]
    drive_expanded = drive.astype(jnp.float32).reshape(batch_rows, channel_groups, -1)
    decay_re, decay_im, in_re, in_im = discretize(lam_re, lam_im, log_dt, in_c)
    push_re = jnp.einsum('bgc,gpc->gpb', drive_expanded, in_re, precision=highest_precision)
    push_im = jnp.einsum('bgc,gpc->gpb', drive_expanded, in_im, precision=highest_precision)
    fresh_real = decay_re[..., None] * states[0] - decay_im[..., None] * states[1] + push_re
    fresh_imaginary = decay_re[..., None] * states[1] + decay_im[..., None] * states[0] + push_im
    readout_rows = jnp.einsum('jyn,jmy->njm', fresh_real, output_coupling[0], precision=highest_precision) - jnp.einsum('jyn,jmy->njm', fresh_imaginary, output_coupling[1], precision=highest_precision) + skip_connection.reshape(channel_groups, -1) * drive_expanded
    readout_rows = readout_rows.reshape(batch_rows, -1)
    gated = (jax.nn.gelu(readout_rows) * jax.nn.sigmoid(gate_pre.astype(jnp.float32))).astype(jnp.bfloat16)
    return (gated, jnp.stack([fresh_real, fresh_imaginary]))

def norm_rows(summed, params):
    wide = summed.astype(jnp.float32)
    mean_row = lax.optimization_barrier(jnp.mean(wide, axis=-1, keepdims=True))
    var_row = lax.optimization_barrier(jnp.mean(wide * wide, axis=-1, keepdims=True)) - mean_row * mean_row
    scaled = (wide - mean_row) * lax.rsqrt(var_row + norm_eps)
    return (scaled * params[0].astype(jnp.float32) + params[1].astype(jnp.float32)).astype(jnp.bfloat16)

def reference(tokens, carried, proj_in, proj_gate, proj_out, norm_params, lambda_re, lambda_im, log_step, in_coupling, out_coupling, skip_gain):
    stream = tokens
    new_states = []
    for layer_idx in range(LAYERS):
        drive = jnp.dot(stream, proj_in[layer_idx], preferred_element_type=jnp.float32).astype(jnp.bfloat16)
        gate_pre = jnp.dot(stream, proj_gate[layer_idx], preferred_element_type=jnp.float32).astype(jnp.bfloat16)
        gated, states = recur(drive, gate_pre, carried[layer_idx], lambda_re[layer_idx], lambda_im[layer_idx], log_step[layer_idx], in_coupling[layer_idx], out_coupling[layer_idx], skip_gain[layer_idx])
        mixed = jnp.dot(gated, proj_out[layer_idx], preferred_element_type=jnp.float32)
        summed = (residual_scale * stream.astype(jnp.float32) + mixed).astype(jnp.bfloat16)
        stream = norm_rows(summed, norm_params[layer_idx])
        new_states.append(states)
    return (stream, jnp.stack(new_states))
```

```python
import jax
import jax.numpy as jnp
from jax import lax
from jax.sharding import PartitionSpec as P

residual_scale = 1.4142135623730951
norm_eps = 1e-05
highest_precision = lax.Precision.HIGHEST
f32, bf16 = jnp.float32, jnp.bfloat16


inner_bits = (1, 4)


def masks_of(bits):
    masks = [0]
    for bit in bits:
        masks += [m | bit for m in masks]
    return masks


def discretize(lam_re, lam_im, log_dt, coupling):
    step_len = jnp.exp(log_dt)[:, None]
    modulus = jnp.exp(lam_re * step_len)
    decay_re = modulus * jnp.cos(lam_im * step_len)
    decay_im = modulus * jnp.sin(lam_im * step_len)
    denominator = lam_re * lam_re + lam_im * lam_im
    shifted = decay_re - 1.0
    coef_re = (shifted * lam_re + decay_im * lam_im) / denominator
    coef_im = (decay_im * lam_re - shifted * lam_im) / denominator
    in_re = coef_re[..., None] * coupling[0] - coef_im[..., None] * coupling[1]
    in_im = coef_re[..., None] * coupling[1] + coef_im[..., None] * coupling[0]
    return (decay_re, decay_im, in_re, in_im)


def recur(drive, gate_pre, states, disc, out_c, skip):
    decay_re, decay_im, in_re, in_im = disc
    groups, entries = decay_re.shape
    batch = drive.shape[1]
    wide = drive.astype(f32).reshape(groups, -1, batch)
    coupling = jnp.concatenate([in_re, in_im], axis=1)
    push = jnp.einsum("gpc,gcb->gpb", coupling, wide, precision=highest_precision)
    fresh_re = decay_re[..., None] * states[0] - decay_im[..., None] * states[1] + push[:, :entries]
    fresh_im = decay_re[..., None] * states[1] + decay_im[..., None] * states[0] + push[:, entries:]
    y = (
        jnp.einsum("gmp,gpb->gmb", out_c[0], fresh_re, precision=highest_precision)
        - jnp.einsum("gmp,gpb->gmb", out_c[1], fresh_im, precision=highest_precision)
        + skip.reshape(groups, -1)[..., None] * wide
    ).reshape(-1, batch)
    gated = (jax.nn.gelu(y) * jax.nn.sigmoid(gate_pre.astype(f32))).astype(bf16)
    return gated, fresh_re, fresh_im


def make_per_device(axis_size):
    inner = masks_of(inner_bits)
    outer = masks_of([1 << i for i in range(axis_size.bit_length() - 1) if (1 << i) not in inner_bits])
    fan = len(inner)
    order = [o ^ i for o in outer for i in inner]

    def swap(x, mask):
        return lax.ppermute(x, "tp", [(i, i ^ mask) for i in range(axis_size)])

    def per_device(
        tokens, carried, proj_in, proj_gate, proj_out, norm_params,
        lambda_re, lambda_im, log_step, in_coupling, out_coupling, skip_gain,
    ):
        layers = proj_in.shape[0]
        batch, width = tokens.shape
        channels = proj_in.shape[2]
        rows = batch // fan
        me = lax.axis_index("tp")
        q = (me & 1) | (((me >> 2) & 1) << 1)

        def part(x, index, size, axis):
            return lax.dynamic_slice_in_dim(x, index * size, size, axis)

        def scatter(x, size, axis):
            return [part(x, q, size, axis)] + [
                swap(part(x, q ^ j, size, axis), inner[j]) for j in range(1, fan)
            ]

        def in_order(pieces, axis):
            stacked = jnp.stack(pieces)
            return jnp.concatenate(
                [lax.dynamic_index_in_dim(stacked, q ^ i, 0, keepdims=False) for i in range(fan)], axis=axis
            )

        def by_place(x, size, axis):
            return jnp.concatenate([part(x, me ^ m, size, axis) for m in order], axis=axis)

        got = jnp.concatenate(scatter(tokens, rows, 0), axis=1)
        half = rows // 2
        top, bottom = got[:half], got[half:]
        held = {0: got}
        tops, bottoms = {0: top}, {0: bottom}
        for bit in [m for m in outer if m and m & (m - 1) == 0][::-1]:
            base = list(tops)
            for m in base:
                tops[m | bit] = swap(tops[m], bit)
            for m in base:
                bottoms[m | bit] = swap(bottoms[m], bit)
        stream = jnp.concatenate(
            [jnp.concatenate([tops[m] for m in outer], axis=1), jnp.concatenate([bottoms[m] for m in outer], axis=1)],
            axis=0,
        )

        both = jnp.concatenate([w[l] for l in range(layers) for w in (proj_in, proj_gate)], axis=1)
        both, _ = lax.optimization_barrier((both, got))
        far = swap(both, inner[2])
        columns = [both, swap(both, inner[1]), far, swap(far, inner[1])]
        span = 2 * channels
        in_whole = [
            by_place(jnp.concatenate([c[:, l * span : (l + 1) * span] for c in columns], axis=1), width, 0)
            for l in range(layers)
        ]

        pad = jnp.zeros((14, width), bf16)
        closing = [jnp.concatenate([proj_out[l], norm_params[l], pad], axis=0) for l in range(layers)]
        ssm = proj_out.shape[1]

        def gather_inner(x):
            away = swap(x, inner[2])
            pair = jnp.concatenate([x, away], axis=-1)
            other = swap(pair, inner[1])
            return [x, other[..., : x.shape[-1]], away, other[..., x.shape[-1] :]]

        def spread_outer(x):
            return [x] + [swap(x, m) for m in outer[1:]]

        closing_whole = []
        for l in range(layers):
            own = closing[l]
            if l + 1 < layers:
                own, _ = lax.optimization_barrier((own, tops[outer[-1]]))
                spread = jnp.concatenate(spread_outer(own), axis=1)
                four = gather_inner(spread)
                whole = jnp.concatenate(
                    [four[j][:, k * width : (k + 1) * width] for k in range(len(outer)) for j in range(fan)], axis=1
                )
            else:
                own, _ = lax.optimization_barrier((own, stream))
                whole = jnp.concatenate(gather_inner(own), axis=1)
            closing_whole.append(
                (by_place(whole[:ssm], channels, 0), whole[ssm].astype(f32), whole[ssm + 1].astype(f32))
            )

        features = width * axis_size
        new_states = []
        for l in range(layers):
            last = l + 1 == layers
            pre = jnp.einsum("rf,fc->cr", stream, in_whole[l], preferred_element_type=f32).astype(bf16)
            mine = [pre[:span]] + [swap(pre[j * span : (j + 1) * span], inner[j]) for j in range(1, fan)]
            mine = in_order(mine, 1)
            disc = discretize(lambda_re[l], lambda_im[l], log_step[l], in_coupling[l])
            gated, fresh_re, fresh_im = recur(
                mine[:channels], mine[channels:], carried[l], disc, out_coupling[l], skip_gain[l]
            )
            new_states.append(jnp.stack([fresh_re, fresh_im]))
            quarter = jnp.concatenate(scatter(gated, rows, 1), axis=0)
            gated_rows = jnp.concatenate(spread_outer(quarter), axis=0)
            out_w, gain, bias = closing_whole[l]
            mixed = jnp.einsum("cr,cn->rn", gated_rows, out_w, preferred_element_type=f32)
            residual = stream[:, : mixed.shape[1]]
            summed = (residual_scale * residual.astype(f32) + mixed).astype(bf16)
            wide = summed.astype(f32)
            sums = jnp.stack([jnp.sum(wide, axis=1), jnp.sum(wide * wide, axis=1)])
            if last:
                parts = spread_outer(sums)
                sums = sum(parts[1:], parts[0])
            sums = sums / features
            mean = sums[0][:, None]
            var = sums[1][:, None] - mean * mean
            stream = ((wide - mean) * lax.rsqrt(var + norm_eps) * gain + bias).astype(bf16)
        back = [stream[:, :width]] + [
            swap(stream[:, j * width : (j + 1) * width], inner[j]) for j in range(1, fan)
        ]
        return in_order(back, 0), jnp.stack(new_states)

    return per_device


def solution(mesh):
    return jax.shard_map(
        make_per_device(mesh.shape["tp"]),
        mesh=mesh,
        in_specs=(
            P("grp", "tp"),
            P(None, None, "tp", None, "grp"),
            P(None, None, "tp"),
            P(None, None, "tp"),
            P(None, None, "tp"),
            P(None, None, "tp"),
            P(None, "tp", None),
            P(None, "tp", None),
            P(None, "tp"),
            P(None, None, "tp", None, None),
            P(None, None, "tp", None, None),
            P(None, "tp"),
        ),
        out_specs=(P("grp", "tp"), P(None, None, "tp", None, "grp")),
        check_vma=False,
    )
```
